32 devices in a mesh: sp: 8 (over z, x), dp: 4 (over y, core).
Axes of the slice: x: 2, y: 2, z: 4, core: 2. Of those that a mesh axis runs over, the one named last changes fastest.
Arguments:
- residual_in: bfloat16 [4, 1024, 2048], P('dp', 'sp'), may hold values from -6 to 6
- ssm_input: bfloat16 [4, 1024, 2048], P('dp', 'sp'), may hold values from -6 to 6
- state_b: bfloat16 [4, 1024, 2048], P('dp', 'sp'), may hold values from -6 to 6
- state_c: bfloat16 [4, 1024, 2048], P('dp', 'sp'), may hold values from -6 to 6
- step_raw: bfloat16 [4, 1024, 64], P('dp', 'sp'), may hold values from -4 to 3
- gate_input: bfloat16 [4, 1024, 2048], P('dp', 'sp'), may hold values from -6 to 6
- conv_x: float32 [7, 2048], P(None, 'sp'), may hold values from -2 to 2
- conv_b: float32 [7, 2048], P(None, 'sp'), may hold values from -2 to 2
- conv_c: float32 [7, 2048], P(None, 'sp'), may hold values from -2 to 2
- decay_rate: float32 [2, 32], P(None, 'sp'), may hold values from 0 to 1, as said below
- mix_gain: float32 [2048], replicated, may hold values from 0.1 to 1.9
- out_weight: bfloat16 [2048, 2048], P('dp'), may hold values from -0.125 to 0.125
- ffn_gain: float32 [2048], replicated, may hold values from 0.1 to 1.9
- routing: int32 [4, 1024, 4], P('dp', 'sp'), may hold values from 0 to 31, all different within a row; in each aligned block of 128 rows (0 to 127, 128 to 255, ..., all dimensions but the last counted through in order) at most 32 rows name the same one
- route_weight: float32 [4, 1024, 4], P('dp', 'sp'), may hold values from 0.1 to 0.6
- gate_w: bfloat16 [32, 2048, 1024], P(('sp', 'dp')), may hold values from -60 to 60
- up_w: bfloat16 [32, 2048, 1024], P(('sp', 'dp')), may hold values from -60 to 60
- down_w: bfloat16 [32, 1024, 2048], P(('sp', 'dp')), may hold values from -0.1875 to 0.1875
Outputs:
- block_out: bfloat16 [4, 1024, 2048], P('dp', 'sp')
The draws below stay inside these ranges and needn't reach their ends.
Inputs may be any that keep to these rules, and one draw needn't show every extreme that they name: `routing`: each row names 4 different experts; within the rows of one device no expert is named by more than 32 rows, a bound that some block reaches. `decay_rate`: Positive.
All inputs are finite; a program needn't handle non-finite values.
Results may differ from the reference program's by a relative error of at most 0.0082.
Values may be sent and summed in bfloat16 or wider, within the bound.
A program may use at most 128 MiB of HBM per device.

```python
import math
import jax
import jax.numpy as jnp
import numpy as np
from jax import lax

D = 2048
HEADS = 32
HEAD_DIM = 64
GROUPS = 16
STATE = 128
CONV = 7
BLOCK = 128
NORM_GROUPS = 4
FF = 1024
TOPK = 4
TOK_DEV = 128
SEQ_LEN = 1024
SEQS = 4
EXPERTS = 32
CAP = 32


def draw_step_raw(key, part):
    noise_key, level_key = jax.random.split(key)
    noise = jnp.clip(jax.random.normal(noise_key, (SEQS, SEQ_LEN, 2 * HEADS), jnp.float32), -3.0, 3.0) * 0.5
    levels = jax.random.uniform(level_key, (SEQS, SEQ_LEN // TOK_DEV, 1, 2 * HEADS), jnp.float32, -2.0, 1.0)
    levels = jnp.broadcast_to(levels, (SEQS, SEQ_LEN // TOK_DEV, TOK_DEV, 2 * HEADS)).reshape(SEQS, SEQ_LEN, 2 * HEADS)
    return (noise + levels).astype(jnp.bfloat16)


def draw_decay_rate(key, part):
    pick_key, fast_key, slow_key = jax.random.split(key, 3)
    share = 0.5
    quick = jax.random.bernoulli(pick_key, share, (2, HEADS))
    fast_rate = jnp.exp(jax.random.uniform(fast_key, (2, HEADS), jnp.float32, math.log(0.02), math.log(0.2)))
    slow_rate = jnp.exp(jax.random.uniform(slow_key, (2, HEADS), jnp.float32, math.log(0.05), 0.0)) / SEQ_LEN
    return jnp.where(quick, fast_rate, slow_rate)


def expert_matrix(key):
    base_key, pick_key = jax.random.split(key)
    values = jnp.clip(jax.random.normal(base_key, (EXPERTS, D, FF), jnp.float32), -6.0, 6.0) * D ** (-0.5)
    values = values * 1.0
    return values


def draw_gate_w(key, part):
    return expert_matrix(jax.random.fold_in(key, 11)).astype(jnp.bfloat16)


def draw_up_w(key, part):
    return expert_matrix(jax.random.fold_in(key, 12)).astype(jnp.bfloat16)


def steps_of(rng, shape, pieces, least, top_value):
    level, own = 1.0, jax.random.fold_in(rng, 6)
    for axis_at, blocks in pieces:
        steps = jnp.exp(jax.random.uniform(jax.random.fold_in(own, axis_at), (blocks,), jnp.float32, least / len(pieces), top_value / len(pieces)))
        level = level * jnp.repeat(steps, shape[axis_at] // blocks).reshape([-1 if axis == axis_at else 1 for axis in range(len(shape))])
    return level


def shared_out(own_key, own, number, rows, amount, top, reach, slope):
    sequence = jax.random.permutation(own_key, amount)
    crowded, common = portions_of(amount, rows * top, reach, slope, True), portions_of(amount, rows * top, reach, slope, False)
    places = jnp.arange(amount)

    def named(tallies, turn):
        used = int((tallies > 0).sum())
        fixed = max(1, used // 4)
        moved = fixed + (places - fixed + turn * (used - fixed)) % max(1, amount - fixed)
        return jnp.zeros((amount,), jnp.int32).at[sequence[jnp.where(places < fixed, places, moved)]].set(jnp.asarray(tallies, jnp.int32))

    tallies = jnp.where(number % 4 == 0, named(crowded, number // 4), named(common, number - number // 4 - 1))
    mixed = jax.random.permutation(jax.random.fold_in(own, 3), amount)
    donor, receiver = mixed[0:amount // 2 * 2:2], mixed[1:amount // 2 * 2:2]
    room = jnp.minimum(tallies[donor] - 1, reach - tallies[receiver]) // 2
    room = jnp.where((donor == sequence[0]) | (receiver == sequence[0]) | (tallies[receiver] == 0), 0, jnp.maximum(room, 0))
    moved = jax.random.randint(jax.random.fold_in(own, 4), (amount // 2,), 0, 1 << 20) % (room + 1)
    tallies = tallies.at[donor].add(-moved).at[receiver].add(moved)
    items = jnp.searchsorted(jnp.cumsum(tallies), jnp.arange(rows * top), side="right").astype(jnp.int32)
    listing = items.reshape(top, rows).T
    listing = listing[jax.random.permutation(jax.random.fold_in(own, 1), rows)]
    turn = jax.random.randint(jax.random.fold_in(own, 2), (rows, 1), 0, top)
    return jnp.take_along_axis(listing, (jnp.arange(top)[None, :] + turn) % top, axis=1)


def portions_of(count, total, limit, skew, full):
    weights = [(1 << 20) // math.isqrt(rank ** skew) + 1 for rank in range(1, count + 1)]
    largest = limit if full else min(limit, max(-(-total // count), total * weights[0] // sum(weights)))
    least = 1 if total - largest >= count - 1 else 0
    holding, spare = [largest] + [least] * (count - 1), total - largest - least * (count - 1)
    while spare > 0:
        movable = [i for i in range(1, count) if holding[i] < largest] or [i for i in range(1, count) if holding[i] < limit]
        mass, budget = sum([weights[i] for i in movable]), spare
        for i in movable:
            addition = min(limit - holding[i], max(1, budget * weights[i] // mass), spare)
            holding[i] = holding[i] + addition
            spare = spare - addition
    return np.array(holding)


def gaussian(own_key, shape, width, limit, shards=(), kind=jnp.bfloat16):
    level = steps_of(own_key, shape, shards, -0.22, 0.18) if shards else 1.0
    values = jax.random.normal(own_key, shape, jnp.float32) * width * level
    return jnp.minimum(jnp.maximum(values, -limit), limit).astype(kind)


def setup_inputs(seed: int = 0) -> dict:
    key_of = jax.random.split(jax.random.key(seed), 19)
    residual_in = gaussian(key_of[0], (SEQS, SEQ_LEN, D), 1.0, 6.0, ((0, 4), (1, 8)))
    ssm_input = gaussian(key_of[1], (SEQS, SEQ_LEN, D), 1.0, 6.0, ((0, 4), (1, 8)))
    state_b = gaussian(key_of[2], (SEQS, SEQ_LEN, GROUPS * STATE), 1.0, 6.0, ((0, 4), (1, 8)))
    state_c = gaussian(key_of[3], (SEQS, SEQ_LEN, GROUPS * STATE), 1.0, 6.0, ((0, 4), (1, 8)))
    step_raw = draw_step_raw(jax.random.fold_in(key_of[18], 71), 0)
    gate_input = gaussian(key_of[5], (SEQS, SEQ_LEN, D), 1.0, 6.0, ((0, 4), (1, 8)))
    conv_x = gaussian(key_of[6], (CONV, D), CONV ** -0.5, 2.0, ((1, 8),), jnp.float32)
    conv_b = gaussian(key_of[7], (CONV, GROUPS * STATE), CONV ** -0.5, 2.0, ((1, 8),), jnp.float32)
    conv_c = gaussian(key_of[8], (CONV, GROUPS * STATE), CONV ** -0.5, 2.0, ((1, 8),), jnp.float32)
    decay_rate = draw_decay_rate(jax.random.fold_in(key_of[18], 71), 0)
    mix_gain = jnp.clip(1.0 + 0.18 * jax.random.normal(key_of[10], (D,), jnp.float32), 0.1, 1.9)
    out_weight = gaussian(key_of[11], (D, D), D ** -0.5, 0.125, ((0, 4),))
    ffn_gain = jnp.clip(1.0 + 0.18 * jax.random.normal(key_of[12], (D,), jnp.float32), 0.1, 1.9)
    routing_keys = jax.random.split(jax.random.fold_in(key_of[13], 1), SEQS * SEQ_LEN // TOK_DEV)
    routing_turns = jax.random.permutation(jax.random.fold_in(key_of[13], 3), SEQS * SEQ_LEN // TOK_DEV)
    routing = jax.vmap(lambda own, number: shared_out(jax.random.fold_in(key_of[13], 2), own, number, TOK_DEV, EXPERTS, TOPK, CAP, 2))(routing_keys, routing_turns).reshape((SEQS, SEQ_LEN, TOPK))
    route_weight = jnp.clip(0.1 + 0.5 * jax.random.uniform(key_of[14], (SEQS, SEQ_LEN, TOPK), jnp.float32) ** steps_of(key_of[14], (SEQS, SEQ_LEN, TOPK), ((0, 4), (1, 8)), -0.2, 0.2), 0.1, 0.6)
    gate_w = draw_gate_w(jax.random.fold_in(key_of[18], 71), 0)
    up_w = draw_up_w(jax.random.fold_in(key_of[18], 71), 0)
    down_w = gaussian(key_of[17], (EXPERTS, FF, D), FF ** -0.5, 0.1875, ((0, 32),))
    return {"residual_in": residual_in, "ssm_input": ssm_input, "state_b": state_b, "state_c": state_c, "step_raw": step_raw, "gate_input": gate_input, "conv_x": conv_x, "conv_b": conv_b, "conv_c": conv_c, "decay_rate": decay_rate, "mix_gain": mix_gain, "out_weight": out_weight, "ffn_gain": ffn_gain, "routing": routing, "route_weight": route_weight, "gate_w": gate_w, "up_w": up_w, "down_w": down_w}


highest = lax.Precision.HIGHEST
epsilon = 1e-05
clamp_limit = 7.0
sigmoid_slope = 1.702
group_rows = 256

def centred_conv(values, taps):
    half_width = taps.shape[0] // 2
    padded = jnp.pad(values, ((half_width, half_width), (0, 0)))
    total = jnp.zeros_like(values)
    for offset in range(taps.shape[0]):
        total = total + padded[offset:offset + values.shape[0]] * taps[offset]
    return total

def ssd_direction(signal, step_size, rates, write_map, read_map):
    length = signal.shape[0]
    head_count = signal.shape[1]
    head_width = signal.shape[2]
    group_count = write_map.shape[1]
    state_width = write_map.shape[2]
    per_group = head_count // group_count
    blocks = length // BLOCK
    scaled = (signal * step_size[..., None]).reshape(blocks, BLOCK, group_count, per_group, head_width)
    cumulative = jnp.cumsum((-step_size * rates).reshape(blocks, BLOCK, group_count, per_group), axis=1)
    write_block = write_map.reshape(blocks, BLOCK, group_count, state_width)
    read_block = read_map.reshape(blocks, BLOCK, group_count, state_width)
    spread = cumulative[:, :, None] - cumulative[:, None]
    lower_mask = (lax.iota(jnp.int32, BLOCK)[:, None] >= lax.iota(jnp.int32, BLOCK)[None, :])[None, :, :, None, None]
    weight_in = jnp.exp(jnp.where(lower_mask, spread, -jnp.inf))
    intersect = jnp.einsum('clgn,csgn->clsg', read_block, write_block, precision=highest)
    inside = jnp.einsum('clsgk,csgkp->clgkp', intersect[..., None] * weight_in, scaled, precision=highest)
    to_end = jnp.exp(cumulative[:, -1:] - cumulative)
    states = jnp.einsum('csgn,csgkp->cgkpn', write_block, scaled * to_end[..., None], precision=highest)
    carry_decay = jnp.exp(cumulative[:, -1])

    def advance(running, block_pair):
        block_state, factor = block_pair
        return (factor[..., None, None] * running + block_state, running)
    initial = jnp.zeros((group_count, per_group, head_width, state_width), jnp.float32)
    _, entering = lax.scan(advance, initial, (states, carry_decay))
    carried = jnp.einsum('clgn,cgkpn->clgkp', read_block, entering, precision=highest) * jnp.exp(cumulative)[..., None]
    return (inside + carried).reshape(length, head_count, head_width)

def both_ways(signal, steps_fwd, steps_bwd, rates, write_map, read_map):
    forward = ssd_direction(signal, steps_fwd, rates[0], write_map, read_map)
    backward = ssd_direction(jnp.flip(signal, 0), jnp.flip(steps_bwd, 0), rates[1], jnp.flip(write_map, 0), jnp.flip(read_map, 0))
    return forward + jnp.flip(backward, 0)

def scale_rows(values, gains):
    return values * lax.rsqrt(lax.optimization_barrier(jnp.mean(values * values, axis=-1, keepdims=True)) + epsilon) * gains

def group_scale(values, gains):
    shaped = values.reshape(values.shape[:-1] + (NORM_GROUPS, values.shape[-1] // NORM_GROUPS))
    shaped = shaped * lax.rsqrt(lax.optimization_barrier(jnp.mean(shaped * shaped, axis=-1, keepdims=True)) + epsilon)
    return shaped.reshape(values.shape) * gains

def expert_apply(rows, gate_mat, up_mat, down_mat):
    gate_value = jnp.minimum(jnp.dot(rows, gate_mat, preferred_element_type=jnp.float32), clamp_limit)
    up_value = jnp.clip(jnp.dot(rows, up_mat, preferred_element_type=jnp.float32), -clamp_limit, clamp_limit)
    active = ((up_value + 1.0) * gate_value * jax.nn.sigmoid(sigmoid_slope * gate_value)).astype(jnp.bfloat16)
    return jnp.dot(active, down_mat, preferred_element_type=jnp.float32).astype(jnp.bfloat16)

def reference(residual_in, ssm_input, state_b, state_c, step_raw, gate_input, conv_x, conv_b, conv_c, decay_rate, mix_gain, out_weight, ffn_gain, routing, route_weight, gate_w, up_w, down_w):

    def mix_sequence(operands):
        signal_in, write_in, read_in, step_in = operands
        length = signal_in.shape[0]
        signal = jax.nn.silu(centred_conv(signal_in.astype(jnp.float32), conv_x)).reshape(length, HEADS, HEAD_DIM)
        write_map = jax.nn.silu(centred_conv(write_in.astype(jnp.float32), conv_b)).reshape(length, GROUPS, STATE)
        read_map = jax.nn.silu(centred_conv(read_in.astype(jnp.float32), conv_c)).reshape(length, GROUPS, STATE)
        step_pair = jax.nn.softplus(step_in.astype(jnp.float32).reshape(length, HEADS, 2))
        result = both_ways(signal, step_pair[..., 0], step_pair[..., 1], decay_rate, write_map, read_map)
        return result.reshape(length, D).astype(jnp.bfloat16)
    mixed_heads = lax.map(mix_sequence, (ssm_input, state_b, state_c, step_raw))
    gated = mixed_heads.astype(jnp.float32) * jax.nn.silu(gate_input.astype(jnp.float32))
    mixed = group_scale(gated, mix_gain).astype(jnp.bfloat16).reshape(-1, D)
    stream = residual_in.reshape(-1, D).astype(jnp.float32) + jnp.dot(mixed, out_weight, preferred_element_type=jnp.float32)
    ffn_input = scale_rows(stream, ffn_gain).astype(jnp.bfloat16)
    flat_expert = routing.reshape(-1).astype(jnp.int32)
    assigned = flat_expert.shape[0]
    flat_token = lax.iota(jnp.int32, assigned) // TOPK
    flat_weight = route_weight.reshape(-1)
    order = jnp.argsort(flat_expert, stable=True).astype(jnp.int32)
    sorted_expert = flat_expert[order]
    counts = jnp.bincount(flat_expert, length=EXPERTS).astype(jnp.int32)
    padded = (counts + group_rows - 1) // group_rows * group_rows
    group_start = jnp.cumsum(counts).astype(jnp.int32) - counts
    padded_end = jnp.cumsum(padded).astype(jnp.int32)
    padded_start = padded_end - padded
    target = padded_start[sorted_expert] + (lax.iota(jnp.int32, assigned) - group_start[sorted_expert])
    block_count = (assigned + EXPERTS * (group_rows - 1)) // group_rows + 1
    total_rows = block_count * group_rows
    row_token = jnp.zeros((total_rows,), jnp.int32).at[target].set(flat_token[order])
    row_weight = jnp.zeros((total_rows,), jnp.float32).at[target].set(flat_weight[order])
    block_expert = jnp.minimum(jnp.searchsorted(padded_end, lax.iota(jnp.int32, block_count) * group_rows, side='right'), EXPERTS - 1).astype(jnp.int32)

    def run_block(routed, block_pair):
        block_index, expert_id = block_pair
        rows_token = lax.dynamic_slice_in_dim(row_token, block_index * group_rows, group_rows)
        rows_weight = lax.dynamic_slice_in_dim(row_weight, block_index * group_rows, group_rows)
        answer = expert_apply(ffn_input[rows_token], gate_w[expert_id], up_w[expert_id], down_w[expert_id])
        return (routed.at[rows_token].add(answer.astype(jnp.float32) * rows_weight[:, None]), None)
    routed_init = jnp.zeros(stream.shape, jnp.float32)
    routed, _ = lax.scan(run_block, routed_init, (lax.iota(jnp.int32, block_count), block_expert))
    return (stream + routed).astype(jnp.bfloat16).reshape(SEQS, SEQ_LEN, D)
```

```python
import functools

import jax
import jax.numpy as jnp
from jax import lax
from jax.experimental import pallas as pl
from jax.experimental.pallas import tpu as pltpu
from jax.sharding import PartitionSpec as P

HEAD_DIM = 64
STATE = 128
BLOCK = 128
NORM_GROUPS = 4
MESH = pl.DeviceIdType.MESH

highest = lax.Precision.HIGHEST
epsilon = 1e-05
clamp_limit = 7.0
sigmoid_slope = 1.702


def greet(peers):
    barrier = pltpu.get_barrier_semaphore()
    for peer in peers:
        pl.semaphore_signal(barrier, inc=1, device_id=peer, device_id_type=MESH)
    pl.semaphore_wait(barrier, len(peers))


def to_heads_kernel(n, *refs):
    srcs, dsts = refs[:4], refs[4:8]
    bounce, step_bounce, send, recv, local = refs[8:]
    me = lax.axis_index("sp")
    rows = srcs[0].shape[0]
    width = dsts[0].shape[1]
    peers = [lax.rem(me + i, n) for i in range(1, n)]
    greet([{"sp": peer} for peer in peers])
    copies = []
    mine = pl.ds(pl.multiple_of(me * rows, rows), rows)
    for i, peer in enumerate(peers):
        for k in range(4):
            if k < 3:
                part = srcs[k].at[:, pl.ds(pl.multiple_of(peer * width, width), width)]
                there = dsts[k].at[mine, :]
            else:
                part = srcs[k]
                there = dsts[k].at[mine, :]
            copy = pltpu.make_async_remote_copy(
                src_ref=part,
                dst_ref=there,
                send_sem=send.at[i, k],
                recv_sem=recv.at[i, k],
                device_id={"sp": peer},
                device_id_type=MESH,
            )
            copy.start()
            copies.append(copy)
    own = [srcs[k].at[:, pl.ds(pl.multiple_of(me * width, width), width)] for k in range(3)]
    own.append(srcs[3])
    slots = [bounce.at[k] for k in range(3)] + [step_bounce]
    first = [pltpu.make_async_copy(own[k], slots[k], local.at[0, k]) for k in range(4)]
    second = [
        pltpu.make_async_copy(slots[k], dsts[k].at[mine, :], local.at[1, k]) for k in range(4)
    ]
    for k in range(4):
        first[k].start()
    for k in range(4):
        first[k].wait()
        second[k].start()
    for k in range(4):
        second[k].wait()
    for copy in copies:
        copy.wait()


def to_heads(n, arrays, steps):
    rows, full = arrays[0].shape
    width = full // n
    wide = jax.ShapeDtypeStruct((rows * n, width), arrays[0].dtype)
    step_out = jax.ShapeDtypeStruct((rows * n, steps.shape[1]), steps.dtype)
    anywhere = pl.BlockSpec(memory_space=pl.ANY)
    return pl.pallas_call(
        functools.partial(to_heads_kernel, n),
        out_shape=(wide, wide, wide, step_out),
        in_specs=[anywhere] * 4,
        out_specs=(anywhere,) * 4,
        scratch_shapes=[
            pltpu.VMEM((3, rows, width), arrays[0].dtype),
            pltpu.VMEM(steps.shape, steps.dtype),
            pltpu.SemaphoreType.DMA((n - 1, 4)),
            pltpu.SemaphoreType.DMA((n - 1, 4)),
            pltpu.SemaphoreType.DMA((2, 4)),
        ],
        compiler_params=pltpu.CompilerParams(collective_id=1, has_side_effects=True),
        name="to_heads",
    )(*arrays, steps)


def to_tokens_kernel(n, src, dst, bounce, send, recv, local):
    me = lax.axis_index("sp")
    rows = dst.shape[0]
    width = src.shape[1]
    peers = [lax.rem(me + i, n) for i in range(1, n)]
    greet([{"sp": peer} for peer in peers])
    there = dst.at[:, pl.ds(pl.multiple_of(me * width, width), width)]
    copies = []
    for i, peer in enumerate(peers):
        copy = pltpu.make_async_remote_copy(
            src_ref=src.at[pl.ds(pl.multiple_of(peer * rows, rows), rows), :],
            dst_ref=there,
            send_sem=send.at[i],
            recv_sem=recv.at[i],
            device_id={"sp": peer},
            device_id_type=MESH,
        )
        copy.start()
        copies.append(copy)
    first = pltpu.make_async_copy(
        src.at[pl.ds(pl.multiple_of(me * rows, rows), rows), :], bounce, local.at[0]
    )
    first.start()
    first.wait()
    second = pltpu.make_async_copy(bounce, there, local.at[1])
    second.start()
    second.wait()
    for copy in copies:
        copy.wait()


def to_tokens(n, heads):
    length, width = heads.shape
    rows = length // n
    anywhere = pl.BlockSpec(memory_space=pl.ANY)
    return pl.pallas_call(
        functools.partial(to_tokens_kernel, n),
        out_shape=jax.ShapeDtypeStruct((rows, n * width), heads.dtype),
        in_specs=[anywhere],
        out_specs=anywhere,
        scratch_shapes=[
            pltpu.VMEM((rows, width), heads.dtype),
            pltpu.SemaphoreType.DMA((n - 1,)),
            pltpu.SemaphoreType.DMA((n - 1,)),
            pltpu.SemaphoreType.DMA((2,)),
        ],
        compiler_params=pltpu.CompilerParams(collective_id=2, has_side_effects=True),
        name="to_tokens",
    )(heads)


def swap_half_kernel(half, dp_count, src, dst, bounce, send, recv, local):
    n = half * dp_count
    first_sp = lax.axis_index("sp") // half * half
    me = lax.rem(lax.axis_index("sp"), half) * dp_count + lax.axis_index("dp")

    def place(peer):
        return {"sp": first_sp + peer // dp_count, "dp": lax.rem(peer, dp_count)}

    barrier = pltpu.get_barrier_semaphore()

    def call(i, carry):
        peer = lax.rem(me + i, n)
        pl.semaphore_signal(barrier, inc=1, device_id=place(peer), device_id_type=MESH)
        return carry

    lax.fori_loop(1, n, call, 0)
    pl.semaphore_wait(barrier, n - 1)

    def remote(i):
        peer = lax.rem(me + i, n)
        return pltpu.make_async_remote_copy(
            src_ref=src.at[peer],
            dst_ref=dst.at[me],
            send_sem=send.at[i - 1],
            recv_sem=recv.at[i - 1],
            device_id=place(peer),
            device_id_type=MESH,
        )

    def begin(i, carry):
        remote(i).start()
        return carry

    lax.fori_loop(1, n, begin, 0)
    first = pltpu.make_async_copy(src.at[me], bounce, local.at[0])
    first.start()
    first.wait()
    second = pltpu.make_async_copy(bounce, dst.at[me], local.at[1])
    second.start()
    second.wait()

    def finish(i, carry):
        remote(i).wait()
        return carry

    lax.fori_loop(1, n, finish, 0)


def swap_half(half, dp_count, rows, identity):
    n = half * dp_count
    anywhere = pl.BlockSpec(memory_space=pl.ANY)
    return pl.pallas_call(
        functools.partial(swap_half_kernel, half, dp_count),
        out_shape=jax.ShapeDtypeStruct(rows.shape, rows.dtype),
        in_specs=[anywhere],
        out_specs=anywhere,
        scratch_shapes=[
            pltpu.VMEM(rows.shape[1:], rows.dtype),
            pltpu.SemaphoreType.DMA((n - 1,)),
            pltpu.SemaphoreType.DMA((n - 1,)),
            pltpu.SemaphoreType.DMA((2,)),
        ],
        compiler_params=pltpu.CompilerParams(collective_id=identity, has_side_effects=True),
        cost_estimate=pl.CostEstimate(flops=10**11, bytes_accessed=rows.size * 4, transcendentals=0),
        name="swap_half_%d" % identity,
    )(rows)


def mixer_kernel(
    x_ref, b_ref, c_ref, tx_ref, tb_ref, tc_ref, st_ref, stt_ref, rate_ref, ratet_ref,
    o_ref, pad, reads, inside_ref, fade_f, fade_b, sums, carry,
):
    length = x_ref.shape[0]
    lanes = x_ref.shape[1]
    blocks = length // BLOCK
    per_group = st_ref.shape[2] // 2
    taps = tx_ref.shape[0]
    half = taps // 2
    f32, bf16 = jnp.float32, jnp.bfloat16
    for k, ref in enumerate((x_ref, b_ref, c_ref)):
        pad[k, 0:8, :] = jnp.zeros((8, lanes), f32)
        pad[k, length + 8 : length + 16, :] = jnp.zeros((8, lanes), f32)
        pad[k, 8 : length + 8, :] = ref[...].astype(f32)

    def conv(k, taps_ref, base):
        total = None
        for j in range(taps):
            term = pad[k, base + 8 - half + j : base + 8 - half + j + BLOCK, :] * taps_ref[j : j + 1, :]
            total = term if total is None else total + term
        return total * jax.nn.sigmoid(total)

    def softplus(v):
        return jnp.maximum(v, 0.0) + jnp.log(1.0 + jnp.exp(-jnp.abs(v)))

    li = lax.broadcasted_iota(jnp.int32, (BLOCK, BLOCK), 0)
    si = lax.broadcasted_iota(jnp.int32, (BLOCK, BLOCK), 1)
    at_or_after = li >= si
    lower = jnp.where(at_or_after, 1.0, 0.0).astype(f32)
    upper = jnp.where(si >= li, 1.0, 0.0).astype(f32)
    lane_head = lax.broadcasted_iota(jnp.int32, (1, lanes), 1) // HEAD_DIM

    def spread_heads(columns):
        out = columns[0]
        for h in range(1, per_group):
            out = jnp.where(lane_head == h, columns[h], out)
        return jnp.broadcast_to(out, (out.shape[0], lanes))

    for c in range(blocks):
        base = c * BLOCK
        rows = slice(base, base + BLOCK)
        x = conv(0, tx_ref, base)
        write = conv(1, tb_ref, base).astype(bf16)
        read = conv(2, tc_ref, base).astype(bf16)
        reads[rows, :] = read
        dt = softplus(st_ref[0, rows, :])
        dtt = softplus(stt_ref[0, :, rows])
        a = dt * rate_ref[0]
        at = dtt * ratet_ref[0]
        inc = jnp.dot(lower, a, precision=highest, preferred_element_type=f32)
        inct = jnp.dot(at, upper, precision=highest, preferred_element_type=f32)
        exc = inc - a
        exct = inct - at
        tot = inc[BLOCK - 1 : BLOCK, :]
        scores = lax.dot_general(
            read, write, (((1,), (1,)), ((), ())), preferred_element_type=f32
        )
        inside = None
        xb = x.astype(bf16)
        for h in range(per_group):
            f, b = 2 * h, 2 * h + 1
            power = jnp.where(
                at_or_after,
                inct[f : f + 1, :] - inc[:, f : f + 1],
                exc[:, b : b + 1] - exct[b : b + 1, :],
            )
            df, db = dtt[f : f + 1, :], dtt[b : b + 1, :]
            scale = jnp.where(li > si, df, jnp.where(li == si, df + db, db))
            weights = (scores * jnp.exp(power) * scale).astype(bf16)
            xh = jnp.where(lane_head == h, x, 0.0).astype(bf16)
            term = jnp.dot(weights, xh, preferred_element_type=f32)
            inside = term if inside is None else inside + term
        inside_ref[rows, :] = inside
        heads = range(per_group)
        fwd = [inc[:, 2 * h : 2 * h + 1] for h in heads]
        bwd = [exc[:, 2 * h + 1 : 2 * h + 2] for h in heads]
        tot_f = [tot[:, 2 * h : 2 * h + 1] for h in heads]
        tot_b = [tot[:, 2 * h + 1 : 2 * h + 2] for h in heads]
        wf = spread_heads([dt[:, 2 * h : 2 * h + 1] * jnp.exp(fwd[h] - tot_f[h]) for h in heads])
        wb = spread_heads([dt[:, 2 * h + 1 : 2 * h + 2] * jnp.exp(-bwd[h]) for h in heads])
        fade_f[rows, :] = spread_heads([jnp.exp(-fwd[h]) for h in heads])
        fade_b[rows, :] = spread_heads([jnp.exp(bwd[h] - tot_b[h]) for h in heads])
        both = jnp.concatenate([(x * wf).astype(bf16), (x * wb).astype(bf16)], axis=1)
        sums[c] = lax.dot_general(
            write, both, (((0,), (0,)), ((), ())), preferred_element_type=f32
        )
        carry[c : c + 1, :] = jnp.concatenate(
            [
                spread_heads([jnp.exp(-tot_f[h]) for h in heads]),
                spread_heads([jnp.exp(-tot_b[h]) for h in heads]),
            ],
            axis=1,
        )

    state = jnp.zeros((sums.shape[1], lanes), f32)
    for c in range(blocks):
        own = sums[c, :, 0:lanes]
        sums[c, :, 0:lanes] = state
        state = carry[c : c + 1, 0:lanes] * state + own
    state = jnp.zeros((sums.shape[1], lanes), f32)
    for c in reversed(range(blocks)):
        own = sums[c, :, lanes : 2 * lanes]
        sums[c, :, lanes : 2 * lanes] = state
        state = carry[c : c + 1, lanes : 2 * lanes] * state + own
    for c in range(blocks):
        rows = slice(c * BLOCK, (c + 1) * BLOCK)
        moved = jnp.dot(reads[rows, :], sums[c].astype(bf16), preferred_element_type=f32)
        total = (
            inside_ref[rows, :]
            + moved[:, 0:lanes] * fade_f[rows, :]
            + moved[:, lanes : 2 * lanes] * fade_b[rows, :]
        )
        o_ref[rows, :] = total.astype(o_ref.dtype)


def mixer(signal, write, read, conv_x, conv_b, conv_c, steps, rates):
    length, width = signal.shape
    groups = write.shape[1] // STATE
    lanes = width // groups
    columns = steps.shape[1] // groups
    taps = conv_x.shape[0]
    blocks = length // BLOCK
    st = steps.astype(jnp.float32).reshape(length, groups, columns).transpose(1, 0, 2)
    stt = st.transpose(0, 2, 1)
    rate = rates.T.reshape(groups, 1, columns)
    ratet = rates.T.reshape(groups, columns, 1)
    wide = pl.BlockSpec((length, lanes), lambda g: (0, g))
    state = pl.BlockSpec((length, STATE), lambda g: (0, g))
    tap_x = pl.BlockSpec((taps, lanes), lambda g: (0, g))
    tap_s = pl.BlockSpec((taps, STATE), lambda g: (0, g))

    def whole(shape):
        return pl.BlockSpec((1,) + shape, lambda g: (g, 0, 0))

    f32 = jnp.float32
    return pl.pallas_call(
        mixer_kernel,
        grid=(groups,),
        out_shape=jax.ShapeDtypeStruct((length, width), jnp.bfloat16),
        in_specs=[
            wide, state, state, tap_x, tap_s, tap_s,
            whole((length, columns)), whole((columns, length)),
            whole((1, columns)), whole((columns, 1)),
        ],
        out_specs=wide,
        scratch_shapes=[
            pltpu.VMEM((3, length + 16, lanes), f32),
            pltpu.VMEM((length, STATE), jnp.bfloat16),
            pltpu.VMEM((length, lanes), f32),
            pltpu.VMEM((length, lanes), f32),
            pltpu.VMEM((length, lanes), f32),
            pltpu.VMEM((blocks, STATE, 2 * lanes), f32),
            pltpu.VMEM((blocks, 2 * lanes), f32),
        ],
        compiler_params=pltpu.CompilerParams(vmem_limit_bytes=40 * 1024 * 1024),
        cost_estimate=pl.CostEstimate(
            flops=40 * 10**9, bytes_accessed=4 * length * width * 2, transcendentals=0
        ),
        name="mixer",
    )(signal, write, read, conv_x, conv_b, conv_c, st, stt, rate, ratet)


def scale_rows(values, gains):
    return values * lax.rsqrt(jnp.mean(values * values, axis=-1, keepdims=True) + epsilon) * gains


def group_scale(values, gains):
    shaped = values.reshape(values.shape[:-1] + (NORM_GROUPS, values.shape[-1] // NORM_GROUPS))
    shaped = shaped * lax.rsqrt(jnp.mean(shaped * shaped, axis=-1, keepdims=True) + epsilon)
    return shaped.reshape(values.shape) * gains


def expert_apply(rows, gate_mat, up_mat, down_mat):
    gate_value = jnp.minimum(
        jnp.dot(rows, gate_mat, preferred_element_type=jnp.float32), clamp_limit
    )
    up_value = jnp.clip(
        jnp.dot(rows, up_mat, preferred_element_type=jnp.float32), -clamp_limit, clamp_limit
    )
    active = ((up_value + 1.0) * gate_value * jax.nn.sigmoid(sigmoid_slope * gate_value)).astype(
        jnp.bfloat16
    )
    return jnp.dot(active, down_mat, preferred_element_type=jnp.float32).astype(jnp.bfloat16)


def gather_rows(weight, count):
    parts = {0: weight}
    step = count // 2
    while step >= 1:
        pairs = [(d, d ^ step) for d in range(count)]
        for offset, block in list(parts.items()):
            parts[offset ^ step] = lax.ppermute(block, "dp", pairs)
        step //= 2
    return parts


def per_device(
    residual_in, ssm_input, state_b, state_c, step_raw, gate_input, conv_x, conv_b, conv_c,
    decay_rate, mix_gain, out_weight, ffn_gain, routing, route_weight, gate_w, up_w, down_w,
):
    sp_count = lax.axis_size("sp")
    dp_count = lax.axis_size("dp")
    bf16, f32 = jnp.bfloat16, jnp.float32
    half = sp_count // 2
    near = half * dp_count
    mirror = [(i, (i + half) % sp_count) for i in range(sp_count)]
    first_expert = lax.axis_index("sp") // half * near
    far_routing = lax.ppermute(routing[0], "sp", mirror)
    far_weight = lax.ppermute(route_weight[0], "sp", mirror)
    parts = gather_rows(out_weight, dp_count)
    signal, write, read, steps = to_heads(
        sp_count, (ssm_input[0], state_b[0], state_c[0]), step_raw[0]
    )
    columns = steps.shape[1] // sp_count
    steps = lax.dynamic_slice_in_dim(steps, lax.axis_index("sp") * columns, columns, axis=1)
    mixed_heads = mixer(signal, write, read, conv_x, conv_b, conv_c, steps, decay_rate)
    mixed_tokens = to_tokens(sp_count, mixed_heads)

    token_count = residual_in.shape[1]
    model_width = residual_in.shape[2]
    gated = mixed_tokens.astype(f32) * jax.nn.silu(gate_input[0].astype(f32))
    mixed = group_scale(gated, mix_gain).astype(bf16)
    depth = out_weight.shape[0]
    me = lax.axis_index("dp")
    stream = residual_in[0].astype(f32)
    for offset, block in parts.items():
        piece = lax.dynamic_slice_in_dim(mixed, (me ^ offset) * depth, depth, axis=1)
        stream = stream + jnp.dot(piece, block, preferred_element_type=f32)
    ffn_input = scale_rows(stream, ffn_gain).astype(bf16)

    top_count = routing.shape[2]
    capacity = 2 * token_count * top_count // (sp_count * dp_count)
    flat = near * capacity
    earlier = (
        lax.iota(jnp.int32, token_count)[:, None] < lax.iota(jnp.int32, token_count)[None, :]
    ).astype(bf16)

    def tables(names, weights):
        chosen = names.T[:, None, :] == (first_expert + lax.iota(jnp.int32, near))[None, :, None]
        named = jnp.any(chosen, axis=0)
        weight_of = jnp.sum(jnp.where(chosen, weights.T[:, None, :], 0.0), axis=0)
        slot = jnp.dot(named.astype(bf16), earlier, preferred_element_type=f32).astype(jnp.int32)
        slot = jnp.where(named, slot, -1)
        pick = slot[:, None, :] == lax.iota(jnp.int32, capacity)[None, :, None]
        high = weight_of.astype(bf16)
        low = (weight_of - high.astype(f32)).astype(bf16)
        zero = jnp.zeros((), bf16)
        combine = jnp.concatenate(
            [
                jnp.where(pick, high[:, None, :], zero).reshape(flat, token_count),
                jnp.where(pick, low[:, None, :], zero).reshape(flat, token_count),
            ],
            axis=1,
        )
        return pick.astype(bf16).reshape(flat, token_count), combine

    def dispatch(select, tokens, identity):
        outgoing = jnp.dot(select, tokens, preferred_element_type=f32).astype(bf16)
        return swap_half(half, dp_count, outgoing.reshape(near, capacity, model_width), identity)

    def serve(arrived):
        return expert_apply(
            arrived.reshape(flat, model_width), gate_w[0], up_w[0], down_w[0]
        ).reshape(arrived.shape)

    def collect(combine, served, identity):
        returned = swap_half(half, dp_count, served, identity)
        sums = lax.dot_general(
            combine, returned.reshape(flat, model_width), (((0,), (0,)), ((), ())),
            preferred_element_type=f32,
        )
        return sums[:token_count] + sums[token_count:]

    select_own, combine_own = tables(routing[0], route_weight[0])
    select_far, combine_far = tables(far_routing, far_weight)
    far_input = lax.ppermute(ffn_input, "sp", mirror)
    arrived_own = dispatch(select_own, ffn_input, 3)
    arrived_far = dispatch(select_far, far_input, 4)
    part_far = collect(combine_far, serve(arrived_far), 5).astype(bf16)
    part_back = lax.ppermute(part_far, "sp", mirror)
    routed = collect(combine_own, serve(arrived_own), 6)
    return (stream + routed + part_back.astype(f32)).astype(bf16)[None]


def solution(mesh):
    return jax.shard_map(
        per_device,
        mesh=mesh,
        in_specs=(
            P("dp", "sp", None),
            P("dp", "sp", None),
            P("dp", "sp", None),
            P("dp", "sp", None),
            P("dp", "sp", None),
            P("dp", "sp", None),
            P(None, "sp"),
            P(None, "sp"),
            P(None, "sp"),
            P(None, "sp"),
            P(),
            P("dp", None),
            P(),
            P("dp", "sp", None),
            P("dp", "sp", None),
            P(("sp", "dp"), None, None),
            P(("sp", "dp"), None, None),
            P(("sp", "dp"), None, None),
        ),
        out_specs=P("dp", "sp", None),
        check_vma=False,
    )
```
